32 devices in a mesh: sp: 16 (over z, y, x), tp: 2 (over core).
Axes of the slice: x: 2, y: 2, z: 4, core: 2. Of those that a mesh axis runs over, the one named last changes fastest.
Arguments:
- resid: bfloat16 [6144, 2048], P(('sp', 'tp')), may hold values from -6 to 6
- q_small: bfloat16 [6144, 1024], P('sp', 'tp'), may hold values from -6 to 6
- k_small: bfloat16 [6144, 1024], P('sp', 'tp'), may hold values from -6 to 6
- v_small: bfloat16 [6144, 1024], P('sp', 'tp'), may hold values from -6 to 6
- q_large: bfloat16 [6144, 1024], P('sp', 'tp'), may hold values from -6 to 6
- k_large: bfloat16 [6144, 1024], P('sp', 'tp'), may hold values from -6 to 6
- v_large: bfloat16 [6144, 1024], P('sp', 'tp'), may hold values from -6 to 6
- gate_small: bfloat16 [6144, 1024], P('sp', 'tp'), may hold values from -6 to 6
- large_head_gate: bfloat16 [6144, 1024], P('sp', 'tp'), may hold values from -6 to 6
- gates_small: float32 [6144, 3, 16], P('sp', None, 'tp'), may hold values from -6 to 300, as said below
- gates_large: float32 [6144, 3, 8], P('sp', None, 'tp'), may hold values from -6 to 300, as said below
- w_out_small: bfloat16 [1024, 2048], P('tp'), may hold values from -0.125 to 0.125
- w_out_large: bfloat16 [1024, 2048], P('tp'), may hold values from -0.125 to 0.125
- norm_gain: float32 [2048], replicated, may hold values from 0.1 to 1.9
- expert_ids: int32 [6144, 2], P(('sp', 'tp')), may hold values from 0 to 15, all different within a row; in each aligned block of 192 rows (0 to 191, 192 to 383, ...) at most 48 rows name the same one
- expert_weight: float32 [6144, 2], P(('sp', 'tp')), may hold values from 0.2 to 1
- w_gate: bfloat16 [16, 2048, 2048], P('sp', None, 'tp'), may hold values from -0.125 to 0.125
- w_up: bfloat16 [16, 2048, 2048], P('sp', None, 'tp'), may hold values from -0.125 to 0.125
- w_down: bfloat16 [16, 2048, 2048], P('sp', 'tp'), may hold values from -0.125 to 0.125
Outputs:
- layer_out: bfloat16 [6144, 2048], P(('sp', 'tp'))
The draws below stay inside these ranges and needn't reach their ends.
Inputs may be any that keep to these rules, and one draw needn't show every extreme that they name: `gates_small`: field 0 is the input gate's pre-activation, field 1 the forget gate's pre-activation, field 2 a non-positive term added to the log forget gate. `gates_large`: field 0 is the input gate's pre-activation, field 1 the forget gate's pre-activation, field 2 a non-positive term added to the log forget gate. `expert_ids`: each row names 2 different experts. In the 192 rows of one device no expert is named by more than 48 rows, and in some device's rows an expert is named exactly 48 times.
All inputs are finite; a program needn't handle non-finite values.
Results may differ from the reference program's by a relative error of at most 0.014.
Values may be sent and summed in bfloat16 or wider, within the bound.
A program may use at most 128 MiB of HBM per device.

```python
import math
import jax
import jax.numpy as jnp
import numpy as np
from jax import lax

D = 2048
HS = 16
DS = 64
HL = 8
DL = 128
FFE = 2048
TOPK = 2
TOK_DEV = 384
ROWS = 192
STEP_COUNT = 6144
EXPERTS = 16
CAP = 48
N_SP = 16
N_TP = 2


def gate_fields(key, head_count):
    concurrent_lanes = jax.random.split(key, 8)
    program_lattice_extent = (STEP_COUNT, head_count)
    log_in = jnp.clip(jax.random.normal(concurrent_lanes[0], program_lattice_extent), -6.0, 6.0)
    fast_share = 0.5
    is_fast = jax.random.uniform(concurrent_lanes[3], (head_count,)) < fast_share
    fast_rate = 1.0 / max(TOK_DEV // 12, 2)
    slow_rate = 0.3 / STEP_COUNT
    base_rate = jnp.where(is_fast, fast_rate, slow_rate)
    block_factor = jnp.exp(jax.random.uniform(concurrent_lanes[4], (STEP_COUNT // TOK_DEV, head_count), minval=-0.7, maxval=0.7))
    block_factor = jnp.repeat(block_factor, TOK_DEV, axis=0)
    noise = jax.random.uniform(concurrent_lanes[5], program_lattice_extent, minval=-1.0, maxval=1.0)
    rate = base_rate[None, :] * block_factor * jnp.exp(noise)
    forget_pre = -jnp.log(jnp.expm1(rate))
    packet_clusters = jax.random.uniform(concurrent_lanes[6], program_lattice_extent) < 4.0 / STEP_COUNT
    discarded_entries = jnp.log(jax.random.uniform(concurrent_lanes[7], program_lattice_extent, minval=0.5, maxval=0.8))
    surplus_quantity = jnp.where(packet_clusters, discarded_entries, 0.0)
    return jnp.stack([log_in, forget_pre, surplus_quantity], axis=1).astype(jnp.float32)


def draw_gates_small(key, part):
    return gate_fields(jax.random.fold_in(key, 11), HS)


def draw_gates_large(key, part):
    return gate_fields(jax.random.fold_in(key, 23), HL)


def block_scale(own_key, shape, cuts, least, top_value):
    level, own = 1.0, jax.random.fold_in(own_key, 6)
    for dim, parts in cuts:
        heights = jnp.exp(jax.random.uniform(jax.random.fold_in(own, dim), (parts,), jnp.float32, least / len(cuts), top_value / len(cuts)))
        level = level * jnp.repeat(heights, shape[dim] // parts).reshape([-1 if axis == dim else 1 for axis in range(len(shape))])
    return level


def routed_block(rng, own, number, rows, count, top, bound, slope):
    order = jax.random.permutation(rng, count)
    heavy_load, ordinary = portions_of(count, rows * top, bound, slope, True), portions_of(count, rows * top, bound, slope, False)
    places = jnp.arange(count)

    def named(lengths, turn):
        used = int((lengths > 0).sum())
        fixed = max(1, used // 4)
        moved = fixed + (places - fixed + turn * (used - fixed)) % max(1, count - fixed)
        return jnp.zeros((count,), jnp.int32).at[order[jnp.where(places < fixed, places, moved)]].set(jnp.asarray(lengths, jnp.int32))

    lengths = jnp.where(number % 4 == 0, named(heavy_load, number // 4), named(ordinary, number - number // 4 - 1))
    mixed = jax.random.permutation(jax.random.fold_in(own, 3), count)
    donor, taker = mixed[0:count // 2 * 2:2], mixed[1:count // 2 * 2:2]
    room = jnp.minimum(lengths[donor] - 1, bound - lengths[taker]) // 2
    room = jnp.where((donor == order[0]) | (taker == order[0]) | (lengths[taker] == 0), 0, jnp.maximum(room, 0))
    moved = jax.random.randint(jax.random.fold_in(own, 4), (count // 2,), 0, 1 << 20) % (room + 1)
    lengths = lengths.at[donor].add(-moved).at[taker].add(moved)
    members = jnp.searchsorted(jnp.cumsum(lengths), jnp.arange(rows * top), side="right").astype(jnp.int32)
    table = members.reshape(top, rows).T
    table = table[jax.random.permutation(jax.random.fold_in(own, 1), rows)]
    turn = jax.random.randint(jax.random.fold_in(own, 2), (rows, 1), 0, top)
    return jnp.take_along_axis(table, (jnp.arange(top)[None, :] + turn) % top, axis=1)


def portions_of(count, total, limit, skew, full):
    portions = [(1 << 20) // math.isqrt(grade ** skew) + 1 for grade in range(1, count + 1)]
    largest = limit if full else min(limit, max(-(-total // count), total * portions[0] // sum(portions)))
    least = 1 if total - largest >= count - 1 else 0
    given, spare = [largest] + [least] * (count - 1), total - largest - least * (count - 1)
    while spare > 0:
        movable = [i for i in range(1, count) if given[i] < largest] or [i for i in range(1, count) if given[i] < limit]
        pool, budget = sum([portions[i] for i in movable]), spare
        for i in movable:
            extra = min(limit - given[i], max(1, budget * portions[i] // pool), spare)
            given[i] = given[i] + extra
            spare = spare - extra
    return np.array(given)


def bell_draw(rng, shape, deviation, reach, pieces=(), held_as=jnp.bfloat16):
    values = jax.random.normal(rng, shape, jnp.float32) * deviation
    if len(pieces) > 0:
        values = block_scale(rng, shape, pieces, -0.22, 0.18) * values
    return jnp.clip(values, min=-reach, max=reach).astype(held_as)


def setup_inputs(seed: int = 0) -> dict:
    key_of = jax.random.split(jax.random.key(seed), 20)
    resid = bell_draw(key_of[0], (STEP_COUNT, D), 1.0, 6.0, ((0, 32),))
    q_small = bell_draw(key_of[1], (STEP_COUNT, HS * DS), 1.0, 6.0, ((0, 16), (1, 2)))
    k_small = bell_draw(key_of[2], (STEP_COUNT, HS * DS), 1.0, 6.0, ((0, 16), (1, 2)))
    v_small = bell_draw(key_of[3], (STEP_COUNT, HS * DS), 1.0, 6.0, ((0, 16), (1, 2)))
    q_large = bell_draw(key_of[4], (STEP_COUNT, HL * DL), 1.0, 6.0, ((0, 16), (1, 2)))
    k_large = bell_draw(key_of[5], (STEP_COUNT, HL * DL), 1.0, 6.0, ((0, 16), (1, 2)))
    v_large = bell_draw(key_of[6], (STEP_COUNT, HL * DL), 1.0, 6.0, ((0, 16), (1, 2)))
    gate_small = bell_draw(key_of[7], (STEP_COUNT, HS * DS), 1.5, 6.0, ((0, 16), (1, 2)))
    large_head_gate = bell_draw(key_of[8], (STEP_COUNT, HL * DL), 1.5, 6.0, ((0, 16), (1, 2)))
    gates_small = draw_gates_small(jax.random.fold_in(key_of[19], 71), 0)
    gates_large = draw_gates_large(jax.random.fold_in(key_of[19], 71), 0)
    w_out_small = bell_draw(key_of[11], (HS * DS, D), (HS * DS + HL * DL) ** -0.5, 0.125, ((0, 2),))
    w_out_large = bell_draw(key_of[12], (HL * DL, D), (HS * DS + HL * DL) ** -0.5, 0.125, ((0, 2),))
    norm_gain = jnp.clip(1.0 + 0.18 * jax.random.normal(key_of[13], (D,), jnp.float32), 0.1, 1.9)
    expert_ids_keys = jax.random.split(jax.random.fold_in(key_of[14], 1), STEP_COUNT // ROWS)
    expert_ids_turns = jax.random.permutation(jax.random.fold_in(key_of[14], 3), STEP_COUNT // ROWS)
    expert_ids = jax.vmap(lambda own, number: routed_block(jax.random.fold_in(key_of[14], 2), own, number, ROWS, EXPERTS, TOPK, CAP, 1))(expert_ids_keys, expert_ids_turns).reshape((STEP_COUNT, TOPK))
    expert_weight = jnp.clip(0.2 + 0.8 * jax.random.uniform(key_of[15], (STEP_COUNT, TOPK), jnp.float32) ** block_scale(key_of[15], (STEP_COUNT, TOPK), ((0, 32),), -0.2, 0.2), 0.2, 1.0)
    w_gate = bell_draw(key_of[16], (EXPERTS, D, FFE), D ** -0.5, 0.125, ((0, 16), (2, 2)))
    w_up = bell_draw(key_of[17], (EXPERTS, D, FFE), D ** -0.5, 0.125, ((0, 16), (2, 2)))
    w_down = bell_draw(key_of[18], (EXPERTS, FFE, D), FFE ** -0.5, 0.125, ((0, 16), (1, 2)))
    return dict(resid=resid, q_small=q_small, k_small=k_small, v_small=v_small, q_large=q_large, k_large=k_large, v_large=v_large, gate_small=gate_small, large_head_gate=large_head_gate, gates_small=gates_small, gates_large=gates_large, w_out_small=w_out_small, w_out_large=w_out_large, norm_gain=norm_gain, expert_ids=expert_ids, expert_weight=expert_weight, w_gate=w_gate, w_up=w_up, w_down=w_down)


floor_neg = -1e+30
norm_eps = 1e-06

def summarize(keys_block, values_block, log_in, log_forget):
    cumulative = jnp.cumsum(log_forget, axis=0)
    totals = cumulative[-1]
    growth = totals[None, :] - cumulative + log_in
    peak_log = lax.optimization_barrier(jnp.max(growth, axis=0))
    factor = jnp.exp(growth - peak_log[None, :])
    scaled = factor[:, :, None] * keys_block.astype(jnp.float32)
    keyed_rows = lax.optimization_barrier(scaled.astype(jnp.bfloat16)).astype(jnp.float32)
    state_mat = jnp.einsum('lhd,lhe->hde', keyed_rows, values_block.astype(jnp.float32))
    state_vec = lax.optimization_barrier(jnp.sum(scaled, axis=0))
    return (state_mat, state_vec, peak_log, totals)

def combine(earlier, later):
    earlier_mat, earlier_vec, earlier_peak, earlier_total = earlier
    later_mat, later_vec, later_peak, later_total = later
    joined = jnp.maximum(earlier_peak + later_total, later_peak)
    earlier_weight = jnp.exp(earlier_peak + later_total - joined)
    later_weight = jnp.exp(later_peak - joined)
    return (earlier_weight[:, None, None] * earlier_mat + later_weight[:, None, None] * later_mat, earlier_weight[:, None] * earlier_vec + later_weight[:, None] * later_vec, joined, earlier_total + later_total)

def read_block(queries, keys_block, values_block, log_in, log_forget, carried):
    state_mat, state_vec, carry_peak, carry_total = carried
    length = queries.shape[0]
    scaling = queries.shape[2] ** (-0.5)
    cumulative = jnp.cumsum(log_forget, axis=0).T
    entries = log_in.T
    positions = jnp.arange(length)
    causal = positions[:, None] >= positions[None, :]
    dlog = jnp.where(causal[None], cumulative[:, :, None] - cumulative[:, None, :] + entries[:, None, :], floor_neg)
    carried_log = cumulative + carry_peak[:, None]
    ceiling = jnp.maximum(carried_log, lax.optimization_barrier(jnp.max(dlog, axis=2)))
    products = jnp.einsum('thd,shd->hts', queries.astype(jnp.float32), keys_block.astype(jnp.float32)) * scaling
    scored = products * jnp.exp(dlog - ceiling[:, :, None])
    scored_b = lax.optimization_barrier(scored.astype(jnp.bfloat16)).astype(jnp.float32)
    carry_weight = jnp.exp(carried_log - ceiling)
    scaled_queries = queries.astype(jnp.float32) * scaling
    numerator = jnp.einsum('hts,shd->htd', scored_b, values_block.astype(jnp.float32))
    numerator = numerator + carry_weight[:, :, None] * jnp.einsum('thd,hde->hte', scaled_queries, state_mat, precision=lax.Precision.HIGHEST)
    denominator = lax.optimization_barrier(jnp.sum(scored, axis=2)) + carry_weight * jnp.einsum('thd,hd->ht', scaled_queries, state_vec, precision=lax.Precision.HIGHEST)
    memory = numerator / jnp.maximum(jnp.abs(denominator), 1.0)[:, :, None]
    return jnp.transpose(memory, (1, 0, 2))

def mix_group(queries, keys, values, out_gate, gates):
    head_count = gates.shape[2]
    head_dim = queries.shape[1] // head_count
    blocks = queries.shape[0] // TOK_DEV
    block_shape = (blocks, TOK_DEV, head_count, head_dim)
    log_in = gates[:, 0, :].reshape(blocks, TOK_DEV, head_count)
    log_forget = (jax.nn.log_sigmoid(gates[:, 1, :]) + gates[:, 2, :]).reshape(blocks, TOK_DEV, head_count)
    initial = (jnp.zeros((head_count, head_dim, head_dim), jnp.float32), jnp.zeros((head_count, head_dim), jnp.float32), jnp.full((head_count,), floor_neg, jnp.float32), jnp.zeros((head_count,), jnp.float32))

    def advance(carried, inputs):
        query_block, key_block, value_block, log_entry, log_keep = inputs
        memory = read_block(query_block, key_block, value_block, log_entry, log_keep, carried)
        return (combine(carried, summarize(key_block, value_block, log_entry, log_keep)), memory)
    _, memory = lax.scan(advance, initial, (queries.reshape(block_shape), keys.reshape(block_shape), values.reshape(block_shape), log_in, log_forget))
    memory = memory.reshape(queries.shape[0], head_count * head_dim)
    return (jax.nn.sigmoid(out_gate.astype(jnp.float32)) * memory).astype(jnp.bfloat16)

def expert_rows(arrived, gate_w, up_w, down_w):
    part_width = gate_w.shape[1] // N_TP
    running = jnp.zeros((arrived.shape[0], down_w.shape[1]), jnp.float32)
    for member in range(N_TP):
        low = member * part_width
        gated = jnp.dot(arrived, gate_w[:, low:low + part_width], preferred_element_type=jnp.float32)
        lifted = jnp.dot(arrived, up_w[:, low:low + part_width], preferred_element_type=jnp.float32)
        hidden = (jax.nn.silu(gated) * lifted).astype(jnp.bfloat16)
        portion = jnp.dot(hidden, down_w[low:low + part_width], preferred_element_type=jnp.float32).astype(jnp.bfloat16)
        running = running + lax.optimization_barrier(portion).astype(jnp.float32)
    return running.astype(jnp.bfloat16)

def reference(resid, q_small, k_small, v_small, q_large, k_large, v_large, gate_small, large_head_gate, gates_small, gates_large, w_out_small, w_out_large, norm_gain, expert_ids, expert_weight, w_gate, w_up, w_down):
    small_out = mix_group(q_small, k_small, v_small, gate_small, gates_small)
    large_out = mix_group(q_large, k_large, v_large, large_head_gate, gates_large)
    small_part = small_out.shape[1] // N_TP
    large_part = large_out.shape[1] // N_TP
    mixed = jnp.zeros((resid.shape[0], resid.shape[1]), jnp.float32)
    for member in range(N_TP):
        low_small = member * small_part
        low_large = member * large_part
        portion = jnp.dot(small_out[:, low_small:low_small + small_part], w_out_small[low_small:low_small + small_part], preferred_element_type=jnp.float32)
        portion = portion + jnp.dot(large_out[:, low_large:low_large + large_part], w_out_large[low_large:low_large + large_part], preferred_element_type=jnp.float32)
        mixed = mixed + lax.optimization_barrier(portion.astype(jnp.bfloat16)).astype(jnp.float32)
    after_mix = resid.astype(jnp.float32) + mixed
    normed = (after_mix * lax.rsqrt(lax.optimization_barrier(jnp.mean(after_mix * after_mix, axis=-1, keepdims=True)) + norm_eps) * norm_gain).astype(jnp.bfloat16)
    sources = N_SP * N_TP
    per_source = ROWS * TOPK
    routed = expert_ids.reshape(sources, per_source).astype(jnp.int32)
    onehot = (routed[:, :, None] == jnp.arange(EXPERTS, dtype=jnp.int32)[None, None, :]).astype(jnp.int32)
    position = lax.optimization_barrier(jnp.sum((jnp.cumsum(onehot, axis=1) - 1) * onehot, axis=2)).astype(jnp.int32)
    route_ids = jnp.arange(sources * per_source, dtype=jnp.int32).reshape(sources, per_source)
    column = jnp.arange(sources, dtype=jnp.int32)[:, None] * CAP + position
    slot_table = jnp.full((EXPERTS, sources * CAP), -1, jnp.int32).at[routed, column].set(route_ids)
    flat_weight = expert_weight.reshape(-1)

    def serve_expert(running, inputs):
        slot_row, gate_w, up_w, down_w = inputs
        filled = slot_row >= 0
        route_id = jnp.where(filled, slot_row, 0)
        token_id = route_id // TOPK
        answer = expert_rows(normed[token_id], gate_w, up_w, down_w).astype(jnp.float32)
        weight = jnp.where(filled, flat_weight[route_id], jnp.zeros((), jnp.float32))
        return (running.at[token_id].add(answer * weight[:, None]), None)
    combined, _ = lax.scan(serve_expert, jnp.zeros(after_mix.shape, jnp.float32), (slot_table, w_gate, w_up, w_down))
    return (after_mix + combined).astype(jnp.bfloat16)
```

```python
import functools

import jax
import jax.numpy as jnp
from jax import lax
from jax.experimental import pallas as pl
from jax.experimental.pallas import tpu as pltpu
from jax.sharding import PartitionSpec as P

floor_neg = -1e30
norm_eps = 1e-06
LANES = 128
MESH = pl.DeviceIdType.MESH
F32 = jnp.float32
BF16 = jnp.bfloat16


def iota(shape, axis):
    return lax.broadcasted_iota(jnp.int32, shape, axis)


def dot(a, b, ca=1, cb=0, **kw):
    return lax.dot_general(
        a, b, (((ca,), (cb,)), ((), ())), preferred_element_type=F32, **kw
    )


def exact_dot(a, b):
    return dot(a, b, precision=lax.Precision.HIGHEST)


def mixer_kernel(
    dims,
    qs, ks, vs, gs, ql, kl, vl, gl,
    lf, lft, li, lit,
    ws, wl, resid, gain, idt, wtt,
    after_ref, out_ref, comb_ref,
    tot_c, tot_a, pre_c, pre_a,
    send_c, send_a, recv_c, recv_a,
    inum, imax, iden, y, psend, precv, own,
    ssem_c, rsem_c, ssem_a, rsem_a, psem,
):
    steps, heads_s, heads_l, experts, capacity = dims
    length = qs.shape[0]
    per = heads_s * LANES // qs.shape[1]
    half = LANES // per
    pairs = heads_s // per
    units = pairs + heads_l
    rows = length // 2
    me = lax.axis_index("sp")
    core = lax.axis_index("tp")
    other = 1 - core

    def partner(step):
        bit = 1 << step
        upper = lax.rem(me // bit, 2)
        return me + bit * (1 - 2 * upper), upper

    barrier = pltpu.get_barrier_semaphore()
    for step in range(steps):
        pl.semaphore_signal(
            barrier, inc=1, device_id={"sp": partner(step)[0]}, device_id_type=MESH
        )
    pl.semaphore_signal(barrier, inc=1, device_id={"tp": other}, device_id_type=MESH)

    lane = iota((1, LANES), 1)

    def spread(columns):
        if len(columns) == 1:
            return jnp.broadcast_to(columns[0], (columns[0].shape[0], LANES))
        picked = columns[0]
        for i in range(1, len(columns)):
            picked = jnp.where(lane >= i * half, columns[i], picked)
        return picked

    def heads_of(unit):
        if unit < pairs:
            return list(range(unit * per, (unit + 1) * per))
        return [heads_s + unit - pairs]

    def view(small, large, unit):
        if unit < pairs:
            return small[:, unit * LANES : (unit + 1) * LANES]
        low = (unit - pairs) * LANES
        return large[:, low : low + LANES]

    def span(unit):
        if unit < pairs:
            return unit * half, half
        return pairs * half + (unit - pairs) * LANES, LANES

    tri = (iota((length, length), 0) >= iota((length, length), 1)).astype(F32)
    upper_tri = (iota((length, length), 0) <= iota((length, length), 1)).astype(F32)
    cum_col = exact_dot(tri, lf[...])
    u_row = lit[...] - exact_dot(lft[...], upper_tri)
    total = cum_col[length - 1 : length, :]
    grow = total - cum_col + li[...]
    peak = jnp.max(grow, axis=0, keepdims=True)
    factor = jnp.exp(grow - peak)

    for unit in range(units):
        hs = heads_of(unit)
        key = view(ks, kl, unit).astype(F32)
        scaled = spread([factor[:, h : h + 1] for h in hs]) * key
        full = dot(scaled.astype(BF16), view(vs, vl, unit), 0, 0)
        low, size = span(unit)
        if unit < pairs:
            packed = full[:half]
            for i in range(1, per):
                packed = jnp.where(lane >= i * half, full[i * half : (i + 1) * half], packed)
        else:
            packed = full
        tot_c[low : low + size, :] = packed
        tot_a[unit : unit + 1, :] = jnp.sum(scaled, axis=0, keepdims=True)
        tot_a[units + unit : units + unit + 1, :] = spread([peak[:, h : h + 1] for h in hs])
        tot_a[2 * units + unit : 2 * units + unit + 1, :] = spread(
            [total[:, h : h + 1] for h in hs]
        )
    pre_c[...] = jnp.zeros_like(pre_c)
    pre_a[...] = jnp.zeros_like(pre_a)
    pre_a[units : 2 * units, :] = jnp.full((units, LANES), floor_neg, F32)

    def copies(step):
        to = {"sp": partner(step)[0]}
        return (
            pltpu.make_async_remote_copy(
                send_c.at[step], recv_c.at[step], ssem_c.at[step], rsem_c.at[step],
                device_id=to, device_id_type=MESH,
            ),
            pltpu.make_async_remote_copy(
                send_a.at[step], recv_a.at[step], ssem_a.at[step], rsem_a.at[step],
                device_id=to, device_id_type=MESH,
            ),
        )

    def send(step):
        send_c[step] = tot_c[...].astype(BF16)
        send_a[step] = tot_a[...]
        for copy in copies(step):
            copy.start()

    def merge(early_c, early_a, late_c, late_a, out_c, out_a):
        em, eb = early_a[units : 2 * units, :], early_a[2 * units :, :]
        lm, lb = late_a[units : 2 * units, :], late_a[2 * units :, :]
        m = jnp.maximum(em + lb, lm)
        ew, lw = jnp.exp(em + lb - m), jnp.exp(lm - m)
        out_a[...] = jnp.concatenate(
            [ew * early_a[:units, :] + lw * late_a[:units, :], m, eb + lb], axis=0
        )
        for unit in range(units):
            low, size = span(unit)
            out_c[low : low + size, :] = (
                ew[unit : unit + 1] * early_c[low : low + size, :].astype(F32)
                + lw[unit : unit + 1] * late_c[low : low + size, :].astype(F32)
            )

    def receive(step):
        for copy in copies(step):
            copy.wait()
        upper = partner(step)[1]
        got_c, got_a = recv_c.at[step], recv_a.at[step]

        @pl.when(upper == 1)
        def _():
            merge(got_c, got_a[...], pre_c, pre_a[...], pre_c, pre_a)
            if step < steps - 1:
                merge(got_c, got_a[...], tot_c, tot_a[...], tot_c, tot_a)

        if step < steps - 1:

            @pl.when(upper == 0)
            def _():
                merge(tot_c, tot_a[...], got_c, got_a[...], tot_c, tot_a)

    block = LANES

    def inner(unit):
        hs = heads_of(unit)
        scale = (half if unit < pairs else LANES) ** (-0.5)
        q, k, v = view(qs, ql, unit), view(ks, kl, unit), view(vs, vl, unit)
        for start in range(0, length, block):
            width = start + block
            causal = iota((block, width), 1) <= iota((block, width), 0) + start
            nums, tops, dens = [], [], []
            for i, h in enumerate(hs):
                q_block = q[start : start + block]
                if len(hs) > 1:
                    mine = (lane >= i * half) & (lane < (i + 1) * half)
                    q_block = jnp.where(mine, q_block, jnp.zeros_like(q_block))
                raw = dot(q_block, k[:width], 1, 1) * scale
                masked = jnp.where(causal, u_row[h : h + 1, :width], floor_neg)
                top = jnp.max(masked, axis=1, keepdims=True)
                scored = raw * jnp.exp(masked - top)
                dens.append(jnp.sum(scored, axis=1, keepdims=True))
                tops.append(top)
                nums.append(dot(scored.astype(BF16), v[:width]))
            num = nums[0]
            for i in range(1, len(hs)):
                num = jnp.where(lane >= i * half, nums[i], num)
            inum[unit, start : start + block, :] = num
            imax[unit, start : start + block, :] = spread(tops)
            iden[unit, start : start + block, :] = spread(dens)

    pl.semaphore_wait(barrier, steps + 1)
    share = -(-units // steps)
    for step in range(steps):
        send(step)
        for unit in range(min(units, step * share), min(units, (step + 1) * share)):
            inner(unit)
        receive(step)

    for unit in range(units):
        hs = heads_of(unit)
        scale = (half if unit < pairs else LANES) ** (-0.5)
        low, size = span(unit)
        q = view(qs, ql, unit)
        state = pre_c[low : low + size, :]
        if unit < pairs:
            state = jnp.concatenate(
                [
                    jnp.where((lane >= i * half) & (lane < (i + 1) * half), state, 0.0)
                    for i in range(per)
                ],
                axis=0,
            )
        inter = dot(q, state.astype(BF16)) * scale
        qn = q.astype(F32) * pre_a[unit : unit + 1, :]
        if len(hs) > 1:
            parts = [
                jnp.sum(
                    jnp.where((lane >= i * half) & (lane < (i + 1) * half), qn, 0.0),
                    axis=1,
                    keepdims=True,
                )
                for i in range(per)
            ]
        else:
            parts = [jnp.sum(qn, axis=1, keepdims=True)]
        inter_den = spread(parts) * scale
        carry_m = pre_a[units + unit : units + unit + 1, :]
        top = jnp.maximum(carry_m, imax[unit])
        own_w, carry_w = jnp.exp(imax[unit] - top), jnp.exp(carry_m - top)
        numer = own_w * inum[unit] + carry_w * inter
        denom = own_w * iden[unit] + carry_w * inter_den
        memory = numer / jnp.maximum(jnp.abs(denom), 1.0)
        gate = jax.nn.sigmoid(view(gs, gl, unit).astype(F32))
        y[:, unit * LANES : (unit + 1) * LANES] = (gate * memory).astype(BF16)

    cut = qs.shape[1]
    features = ws.shape[1]
    step_n = 512

    def project(which, dst):
        low = pl.multiple_of(which * rows, 16)
        left = y[pl.ds(low, rows), :cut]
        right = y[pl.ds(low, rows), cut:]
        for n in range(0, features, step_n):
            dst[:, n : n + step_n] = (
                dot(left, ws[:, n : n + step_n]) + dot(right, wl[:, n : n + step_n])
            ).astype(BF16)

    project(other, psend)
    swap = pltpu.make_async_remote_copy(
        psend, precv, psem.at[0], psem.at[1], device_id={"tp": other}, device_id_type=MESH
    )
    swap.start()
    project(core, own)

    expert = iota((experts, rows), 0)
    first, second = idt[0:1, :] == expert, idt[1:2, :] == expert
    hit = (first | second).astype(BF16)
    weight = jnp.where(first, wtt[0:1, :], 0.0) + jnp.where(second, wtt[1:2, :], 0.0)
    before = (iota((rows, rows), 0) < iota((rows, rows), 1)).astype(BF16)
    count = dot(hit, before)
    slots = experts * capacity
    slot = iota((slots, 1), 0).astype(F32)
    group = jnp.floor((slot + 0.5) * (1.0 / capacity))
    place = slot - group * capacity
    member = (group == iota((slots, experts), 1).astype(F32)).astype(BF16)
    chosen = (dot(member, hit) > 0.5) & (dot(member, count.astype(BF16)) == place)
    select = chosen.astype(BF16)
    comb_ref[...] = jnp.where(chosen, dot(member, weight.astype(BF16)), 0.0).astype(BF16)

    swap.wait()
    after = resid[...].astype(F32) + (own[...].astype(F32) + precv[...].astype(F32))
    after_ref[...] = after
    normed = (
        after * lax.rsqrt(jnp.mean(after * after, axis=-1, keepdims=True) + norm_eps) * gain[...]
    ).astype(BF16)
    for n in range(0, features, step_n):
        out_ref[:, n : n + step_n] = dot(select, normed[:, n : n + step_n]).astype(BF16)


def mixer(args, experts, capacity):
    (resid, qs, ks, vs, ql, kl, vl, gs, gl, gates_s, gates_l, ws, wl, gain, ids, weights) = args
    length = qs.shape[0]
    heads_s, heads_l = gates_s.shape[2], gates_l.shape[2]
    steps = lax.axis_size("sp").bit_length() - 1
    gates = jnp.concatenate([gates_s, gates_l], axis=2)
    gates = jnp.pad(gates, ((0, 0), (0, 0), (0, -gates.shape[2] % 8)))
    li = gates[:, 0]
    lf = jax.nn.log_sigmoid(gates[:, 1]) + gates[:, 2]
    rows, features = resid.shape
    half = qs.shape[1] // heads_s
    pairs = qs.shape[1] // LANES
    units = pairs + heads_l
    state = pairs * half + heads_l * LANES
    vm = pl.BlockSpec(memory_space=pltpu.VMEM)
    slots = experts * capacity
    return pl.pallas_call(
        functools.partial(mixer_kernel, (steps, heads_s, heads_l, experts, capacity)),
        out_shape=(
            jax.ShapeDtypeStruct((rows, features), F32),
            jax.ShapeDtypeStruct((slots, features), BF16),
            jax.ShapeDtypeStruct((slots, rows), BF16),
        ),
        in_specs=[vm] * 18,
        out_specs=(vm, vm, vm),
        scratch_shapes=[
            pltpu.VMEM((state, LANES), F32),
            pltpu.VMEM((3 * units, LANES), F32),
            pltpu.VMEM((state, LANES), F32),
            pltpu.VMEM((3 * units, LANES), F32),
            pltpu.VMEM((steps, state, LANES), BF16),
            pltpu.VMEM((steps, 3 * units, LANES), F32),
            pltpu.VMEM((steps, state, LANES), BF16),
            pltpu.VMEM((steps, 3 * units, LANES), F32),
            pltpu.VMEM((units, length, LANES), F32),
            pltpu.VMEM((units, length, LANES), F32),
            pltpu.VMEM((units, length, LANES), F32),
            pltpu.VMEM((length, units * LANES), BF16),
            pltpu.VMEM((rows, features), BF16),
            pltpu.VMEM((rows, features), BF16),
            pltpu.VMEM((rows, features), BF16),
            pltpu.SemaphoreType.DMA((steps,)),
            pltpu.SemaphoreType.DMA((steps,)),
            pltpu.SemaphoreType.DMA((steps,)),
            pltpu.SemaphoreType.DMA((steps,)),
            pltpu.SemaphoreType.DMA((2,)),
        ],
        compiler_params=pltpu.CompilerParams(collective_id=0, has_side_effects=True),
        cost_estimate=pl.CostEstimate(
            flops=40_000_000_000, bytes_accessed=16_000_000, transcendentals=0
        ),
        name="mixer",
    )(
        qs, ks, vs, gs, ql, kl, vl, gl,
        lf, lf.T, li, li.T,
        ws, wl, resid, gain.reshape(1, -1), ids.T, weights.T,
    )


def expert_part(arrived, gate_w, up_w, down_w):
    gated = jnp.dot(arrived, gate_w, preferred_element_type=F32)
    lifted = jnp.dot(arrived, up_w, preferred_element_type=F32)
    hidden = (jax.nn.silu(gated) * lifted).astype(BF16)
    return jnp.dot(hidden, down_w, preferred_element_type=F32)


def body(*args):
    w_gate, w_up, w_down = args[16:]
    experts = w_gate.shape[0] * lax.axis_size("sp")
    tok_dev = args[1].shape[0]
    capacity = max(2, tok_dev * args[14].shape[1] // experts)
    own_w = (w_gate[0], w_up[0], w_down[0])
    swap = [(0, 1), (1, 0)]
    other_w = tuple(lax.ppermute(w, "tp", swap) for w in own_w)
    after, outgoing, comb = mixer(args[:16], experts, capacity)
    features = outgoing.shape[1]
    arrived = lax.all_to_all(
        outgoing.reshape(experts, capacity, features), "sp", 0, 0, tiled=True
    )
    flattened = arrived.reshape(-1, features)
    running = expert_part(flattened, *own_w) + expert_part(flattened, *other_w)
    answered = running.astype(BF16).reshape(arrived.shape)
    returned = lax.all_to_all(answered, "sp", 0, 0, tiled=True).reshape(-1, features)
    combined = lax.dot_general(
        comb, returned, (((0,), (0,)), ((), ())), preferred_element_type=F32
    )
    return (after + combined).astype(BF16)


def solution(mesh):
    return jax.shard_map(
        body,
        mesh=mesh,
        in_specs=(
            P(("sp", "tp"), None),
            P("sp", "tp"),
            P("sp", "tp"),
            P("sp", "tp"),
            P("sp", "tp"),
            P("sp", "tp"),
            P("sp", "tp"),
            P("sp", "tp"),
            P("sp", "tp"),
            P("sp", None, "tp"),
            P("sp", None, "tp"),
            P("tp", None),
            P("tp", None),
            P(),
            P(("sp", "tp"), None),
            P(("sp", "tp"), None),
            P("sp", None, "tp"),
            P("sp", None, "tp"),
            P("sp", "tp", None),
        ),
        out_specs=P(("sp", "tp"), None),
        check_vma=False,
    )
```
